768 devices in a mesh: fs: 96 (over z, y), tp: 8 (over x, core).
Axes of the slice: x: 4, y: 8, z: 12, core: 2. Of those that a mesh axis runs over, the one named last changes fastest.
Arguments:
- inputs: bfloat16 [49152, 2112], P('fs', 'tp'), may hold values from -20 to 20
- w_conv_up: bfloat16 [2112, 2816], P('fs', 'tp'), may hold values from -0.125 to 0.125
- w_gate_up: bfloat16 [2112, 2816], P('fs', 'tp'), may hold values from -0.125 to 0.125
- w_down: bfloat16 [2816, 2112], P('tp', 'fs'), may hold values from -0.109375 to 0.109375
- taps: float32 [3, 2816], replicated, may hold values from -3 to 3
- conv_bias: float32 [2816], replicated, may hold values from -3 to 3
- cotangent: bfloat16 [49152, 2112], P('fs', 'tp'), may hold values from -6 to 6
Outputs:
- grad_inputs: bfloat16 [49152, 2112], P('fs', 'tp')
- grad_conv_up: float32 [2112, 2816], P('fs', 'tp')
- unit_norms: float32 [2816], P('tp')
- grad_taps: float32 [3, 2816], replicated
- grad_bias: float32 [2816], replicated
The draws below stay inside these ranges and needn't reach their ends.
All inputs are finite; a program needn't handle non-finite values.
Results may differ from the reference program's by a relative error of at most 0.018.
Values may be sent and summed in bfloat16 or wider, within the bound.
No kernel may reach another device: no remote copies, remote signals or barrier semaphores. Data moves between devices by JAX's collectives and lax.ppermute only.
A program may use at most 64 MiB of HBM per device.

```python
import math
import jax
import jax.numpy as jnp
from jax import lax

D = 2112
FF = 2816
TAPS = 3
TOKENS = 49152
N_TP = 8


def with_spikes(entries, key, source, target, shards_of, factor):
    def block_of(dim):
        return (jnp.arange(entries.shape[dim]) // (entries.shape[dim] // shards_of)).reshape((-1,) + (1,) * (entries.ndim - 1 - dim))

    near = jax.random.permutation(key, shards_of)[block_of(target)]
    other_side = (block_of(target) + shards_of // 2) % shards_of
    return jnp.where((block_of(source) == near) | (block_of(source) == other_side), factor * entries, entries)


def shard_levels(key, extent, split, smallest, high):
    def one(dim, blocks):
        steps = jax.random.uniform(jax.random.fold_in(jax.random.fold_in(key, 6), dim), (blocks,), jnp.float32, smallest / len(split), high / len(split))
        return jnp.repeat(jnp.exp(steps), extent[dim] // blocks).reshape((-1,) + (1,) * (len(extent) - dim - 1))

    level = one(*split[0])
    for cut in split[1:]:
        level = level * one(*cut)
    return level


def gaussian(own_key, dims, scale, reach, cuts=(), kind=jnp.bfloat16):
    level = shard_levels(own_key, dims, cuts, -0.22, 0.18) if cuts else 1.0
    result = jax.random.normal(own_key, dims, jnp.float32) * scale * level
    return jnp.minimum(jnp.maximum(result, -reach), reach).astype(kind)


def heavy_noise(stream_key, extent, deviation, limit, cuts, heavy, held_as=jnp.bfloat16):
    entries = deviation * jax.random.normal(stream_key, extent, jnp.float32)
    if cuts:
        entries = entries * shard_levels(stream_key, extent, cuts, -0.22, 0.18)
    return jnp.clip(with_spikes(entries, jax.random.fold_in(stream_key, 3), *heavy), -limit, limit).astype(held_as)


def setup_inputs(seed: int = 0) -> dict:
    key_list = jax.random.split(jax.random.key(seed), 8)
    return {
        "inputs": heavy_noise(key_list[0], (TOKENS, D), 1.0, 20.0, ((0, 96), (1, 8)), (0, 1, 96, 4.75)),
        "w_conv_up": gaussian(key_list[1], (D, FF), D ** -0.5, 0.125, ((0, 96), (1, 8))),
        "w_gate_up": gaussian(key_list[2], (D, FF), D ** -0.5, 0.125, ((0, 96), (1, 8))),
        "w_down": gaussian(key_list[3], (FF, D), FF ** -0.5, 0.109375, ((0, 8), (1, 96))),
        "taps": gaussian(key_list[4], (TAPS, FF), 0.6, 3.0, (), jnp.float32),
        "conv_bias": gaussian(key_list[5], (FF,), 0.5, 3.0, (), jnp.float32),
        "cotangent": gaussian(key_list[6], (TOKENS, D), 1.0, 6.0, ((0, 96), (1, 8))),
    }


def gelu_parts(value):
    normal_cdf = 0.5 * (1.0 + jax.scipy.special.erf(value / math.sqrt(2.0)))
    density = jnp.exp(-0.5 * value * value) / math.sqrt(2.0 * math.pi)
    return (value * normal_cdf, normal_cdf + value * density)

def reference(inputs, w_conv_up, w_gate_up, w_down, taps, conv_bias, cotangent):
    span = TAPS - 1
    rows = inputs.shape[0]
    up_a = jnp.dot(inputs, w_conv_up, preferred_element_type=jnp.float32).astype(jnp.bfloat16)
    up_b = jnp.dot(inputs, w_gate_up, preferred_element_type=jnp.float32).astype(jnp.bfloat16)
    extended = jnp.concatenate([jnp.zeros((span, FF), jnp.float32), up_a.astype(jnp.float32)], 0)
    conv_out = conv_bias[None, :] + sum((taps[i][None, :] * extended[i:i + rows] for i in range(TAPS)))
    d_hidden = jnp.dot(cotangent, w_down.T, preferred_element_type=jnp.float32).astype(jnp.bfloat16)
    gelu_value, gelu_slope = gelu_parts(conv_out)
    d_conv = d_hidden.astype(jnp.float32) * up_b.astype(jnp.float32) * gelu_slope
    d_up_b = (d_hidden.astype(jnp.float32) * gelu_value).astype(jnp.bfloat16)
    d_extended = jnp.concatenate([d_conv, jnp.zeros((span, FF), jnp.float32)], 0)
    d_up_a = sum((taps[i][None, :] * d_extended[span - i:span - i + rows] for i in range(TAPS))).astype(jnp.bfloat16)
    grad_taps = jnp.stack([lax.optimization_barrier(jnp.sum(d_conv * extended[i:i + rows], axis=0)) for i in range(TAPS)], 0)
    grad_bias = lax.optimization_barrier(jnp.sum(d_conv, axis=0))
    group = FF // N_TP
    total = jnp.zeros((rows, D), jnp.float32)
    for k in range(N_TP):
        lo = k * group
        part = jnp.dot(d_up_a[:, lo:lo + group], w_conv_up[:, lo:lo + group].T, preferred_element_type=jnp.float32)
        part = part + jnp.dot(d_up_b[:, lo:lo + group], w_gate_up[:, lo:lo + group].T, preferred_element_type=jnp.float32)
        total = total + part.astype(jnp.bfloat16).astype(jnp.float32)
    grad_inputs = total.astype(jnp.bfloat16)
    grad_conv_up = jnp.dot(inputs.T, d_up_a, preferred_element_type=jnp.float32)
    unit_norms = lax.optimization_barrier(jnp.sum(grad_conv_up * grad_conv_up, axis=0))
    return (grad_inputs, grad_conv_up, unit_norms, grad_taps, grad_bias)
```

```python
import math

import jax
import jax.numpy as jnp
from jax import lax
from jax.sharding import Mesh
from jax.sharding import PartitionSpec as P

TAPS = 3
FS = ("z", "y")
TP = ("x", "c")
LANES = 128


def up_to(n, m):
    return -(-n // m) * m


def pad_to(value, dim, length):
    widths = [(0, 0)] * value.ndim
    widths[dim] = (0, length - value.shape[dim])
    return jnp.pad(value, widths)


def broadcast(value, axes):
    copies = jnp.broadcast_to(value, (lax.axis_size(axes), *value.shape))
    return lax.all_to_all(copies, axes, split_axis=0, concat_axis=0, tiled=True)


def neighbour(block, distance):
    devices = range(lax.axis_size(FS))
    route = [(i - distance, i) for i in devices if i - distance in devices]
    return lax.ppermute(block, FS, route)


def gelu_parts(value):
    normal_cdf = 0.5 * (1.0 + jax.scipy.special.erf(value / math.sqrt(2.0)))
    density = jnp.exp(-0.5 * value * value) / math.sqrt(2.0 * math.pi)
    return (value * normal_cdf, normal_cdf + value * density)


def per_device(inputs, w_conv_up, w_gate_up, w_down, taps, conv_bias, cotangent):
    span = TAPS - 1
    nz, ny = lax.axis_size("z"), lax.axis_size("y")
    ntp = lax.axis_size(TP)
    rows, feats = inputs.shape
    wrows, width = w_conv_up.shape
    wpad, fpad = up_to(wrows, 8), up_to(width, LANES)
    groups = feats // wrows
    f32 = jnp.float32

    before = neighbour(inputs[rows - span :], 1)
    after = neighbour(jnp.concatenate([inputs[:span], cotangent[:span]], 0), -1)

    packed = jnp.concatenate(
        [pad_to(w, 1, fpad) for w in (w_conv_up, w_gate_up, w_down.T)], axis=1
    )
    packed = pad_to(packed, 0, wpad)
    over_y = broadcast(packed, "y").reshape(ny * wpad, 3 * fpad)
    weights = lax.all_gather(over_y, "z", axis=0, tiled=True)

    halo = pad_to(jnp.concatenate([before, after], 0), 0, LANES)
    acts = jnp.concatenate([inputs, halo, cotangent], 0).T
    acts = pad_to(acts.reshape(groups, wrows, -1), 1, wpad)
    acts, over_y = lax.optimization_barrier((acts, over_y))
    tokens = acts.shape[-1]
    over_x = broadcast(acts, "x")
    over_tp = broadcast(over_x, "c")
    whole = jnp.moveaxis(over_tp, 0, 1).reshape(nz * ny, wpad, tokens)
    by_y = whole[:, :, :rows].reshape(nz, ny, wpad, rows)
    by_y = jnp.moveaxis(by_y, 0, 1).reshape(ny * nz * wpad, rows)
    whole = whole.reshape(nz * ny * wpad, tokens)

    start = lax.axis_index(TP) * width
    taps_own = pad_to(lax.dynamic_slice_in_dim(taps, start, width, 1), 1, fpad)
    bias_own = pad_to(lax.dynamic_slice_in_dim(conv_bias, start, width, 0), 0, fpad)

    def over_rows(a, b):
        return lax.dot_general(a, b, (((0,), (0,)), ((), ())), preferred_element_type=f32)

    ups = over_rows(whole[:, : rows + LANES], weights[:, : 2 * fpad]).astype(jnp.bfloat16)
    d_hid = over_rows(whole[:, rows:], weights[:, 2 * fpad :]).astype(jnp.bfloat16)
    up_a, up_b = ups[:, :fpad].astype(f32), ups[:, fpad:].astype(f32)
    first = rows + span
    extended = jnp.concatenate([up_a[rows:first], up_a[:rows], up_a[first : first + span]], 0)
    gate = jnp.concatenate([up_b[:rows], up_b[first : first + span]], 0)
    hidden_grad = jnp.concatenate(
        [d_hid[LANES:], d_hid[2 * span : 3 * span]], 0
    ).astype(f32)
    reach = rows + span
    conv_out = bias_own[None, :] + sum(
        (taps_own[i][None, :] * extended[i : i + reach] for i in range(TAPS))
    )
    gelu_value, gelu_slope = gelu_parts(conv_out)
    d_conv = hidden_grad * gate * gelu_slope
    d_up_b = (hidden_grad[:rows] * gelu_value[:rows]).astype(jnp.bfloat16)
    d_up_a = sum(
        (taps_own[i][None, :] * d_conv[span - i : span - i + rows] for i in range(TAPS))
    ).astype(jnp.bfloat16)
    own = d_conv[:rows]
    sums = [jnp.sum(own * extended[i : i + rows], axis=0) for i in range(TAPS)]
    sums.append(jnp.sum(own, axis=0))

    both = jnp.concatenate([d_up_a, d_up_b], 1)
    partial = lax.dot_general(
        weights[:, : 2 * fpad], both, (((1,), (1,)), ((), ())), preferred_element_type=f32
    ).astype(jnp.bfloat16)
    grad_in = lax.psum_scatter(partial, TP, scatter_dimension=0, tiled=True)
    grad_in = grad_in.reshape(groups, wpad, rows)[:, :wrows].reshape(feats, rows).T

    part = jnp.dot(by_y, d_up_a, preferred_element_type=f32).astype(jnp.bfloat16)
    part = part.reshape(ny, nz * wpad, fpad)
    part = lax.all_to_all(part, "y", split_axis=0, concat_axis=0, tiled=True)
    part = jnp.sum(part.astype(f32), axis=0).reshape(nz, wpad, fpad)
    part = lax.all_to_all(part, "z", split_axis=0, concat_axis=0, tiled=True)
    grad_up = jnp.sum(part, axis=0)

    small = jnp.stack([jnp.sum(grad_up * grad_up, axis=0)] + sums, 0)
    small = pad_to(small, 0, 8)
    small = jnp.sum(broadcast(small, "z"), axis=0)
    small = broadcast(small, ("y", *TP)).reshape(ny, ntp, 8, fpad)
    small = jnp.sum(small, axis=0)[:, :, :width]
    unit_norms = lax.dynamic_index_in_dim(small, lax.axis_index(TP), 0, keepdims=False)[0]
    columns = jnp.moveaxis(small[:, 1 : TAPS + 2], 0, 1).reshape(TAPS + 1, ntp * width)
    return (grad_in, grad_up[:wrows, :width], unit_norms, columns[:TAPS], columns[TAPS])


def solution(mesh):
    finer = Mesh(mesh.devices.reshape(12, 8, 4, 2), ("z", "y", "x", "c"))
    placed = (P(FS, TP), P(FS, TP), P(FS, TP), P(TP, FS), P(), P(), P(FS, TP))
    return jax.shard_map(
        per_device,
        mesh=finer,
        in_specs=placed,
        out_specs=(P(FS, TP), P(FS, TP), P(TP), P(), P()),
        check_vma=False,
    )
```

```python
import math

import jax
import jax.numpy as jnp
from jax import lax
from jax.sharding import Mesh
from jax.sharding import PartitionSpec as P


TAPS = 3
FS = ("z", "y")
TP = ("x", "c")
LANES = 128


def up_to(n, m):
    return -(-n // m) * m


def pad_to(value, dim, length):
    widths = [(0, 0)] * value.ndim
    widths[dim] = (0, length - value.shape[dim])
    return jnp.pad(value, widths)


def broadcast(value, axes):
    copies = jnp.broadcast_to(value, (lax.axis_size(axes), *value.shape))
    return lax.all_to_all(copies, axes, split_axis=0, concat_axis=0, tiled=True)


def exchange(value, axis):
    return lax.all_to_all(value, axis, split_axis=0, concat_axis=0, tiled=True)


def total(parts, kind):
    return sum(parts[i].astype(jnp.float32) for i in range(parts.shape[0])).astype(kind)


def neighbour(block, distance):
    devices = range(lax.axis_size(FS))
    route = [(i - distance, i) for i in devices if i - distance in devices]
    return lax.ppermute(block, FS, route)


def gelu_parts(value):
    normal_cdf = 0.5 * (1.0 + jax.scipy.special.erf(value / math.sqrt(2.0)))
    density = jnp.exp(-0.5 * value * value) / math.sqrt(2.0 * math.pi)
    return (value * normal_cdf, normal_cdf + value * density)


def per_device(inputs, w_conv_up, w_gate_up, w_down, taps, conv_bias, cotangent):
    span = TAPS - 1
    nz, ny = lax.axis_size("z"), lax.axis_size("y")
    ntp = lax.axis_size(TP)
    rows, feats = inputs.shape
    wrows, width = w_conv_up.shape
    fpad = up_to(width, LANES)
    f32 = jnp.float32

    packed = jnp.concatenate(
        [pad_to(w, 1, fpad) for w in (w_conv_up, w_gate_up, w_down.T)], axis=1
    )
    over_y = broadcast(packed, "y").reshape(ny * wrows, 3 * fpad)
    weights = lax.all_gather(over_y, "z", axis=0, tiled=True)

    before = neighbour(inputs[rows - span :], 1)
    after = neighbour(jnp.concatenate([inputs[:span], cotangent[:span]], 0), -1)

    halo = pad_to(jnp.concatenate([before, after], 0), 0, LANES)
    acts = jnp.concatenate([inputs, halo, cotangent], 0).T
    acts, over_y = lax.optimization_barrier((acts, over_y))
    tokens = acts.shape[-1]
    over_tp = broadcast(broadcast(acts, "x"), "c")
    whole = jnp.moveaxis(over_tp, 0, 1).reshape(ntp * feats, tokens)
    by_y = whole[:, :rows].reshape(nz, ny, wrows, rows)
    by_y = jnp.moveaxis(by_y, 0, 1).reshape(ny * nz * wrows, rows)

    start = lax.axis_index(TP) * width
    taps_own = pad_to(lax.dynamic_slice_in_dim(taps, start, width, 1), 1, fpad)
    bias_own = pad_to(lax.dynamic_slice_in_dim(conv_bias, start, width, 0), 0, fpad)

    def over_rows(a, b):
        return lax.dot_general(a, b, (((0,), (0,)), ((), ())), preferred_element_type=f32)

    whole, by_y, taps_own, bias_own, weights = lax.optimization_barrier(
        (whole, by_y, taps_own, bias_own, weights)
    )
    ups = over_rows(whole[:, : rows + LANES], weights[:, : 2 * fpad]).astype(jnp.bfloat16)
    d_hid = over_rows(whole[:, rows:], weights[:, 2 * fpad :]).astype(jnp.bfloat16)
    up_a, up_b = ups[:, :fpad].astype(f32), ups[:, fpad:].astype(f32)
    first = rows + span
    extended = jnp.concatenate([up_a[rows:first], up_a[:rows], up_a[first : first + span]], 0)
    gate = jnp.concatenate([up_b[:rows], up_b[first : first + span]], 0)
    hidden_grad = jnp.concatenate(
        [d_hid[LANES:], d_hid[2 * span : 3 * span]], 0
    ).astype(f32)
    reach = rows + span
    conv_out = bias_own[None, :] + sum(
        (taps_own[i][None, :] * extended[i : i + reach] for i in range(TAPS))
    )
    gelu_value, gelu_slope = gelu_parts(conv_out)
    d_conv = hidden_grad * gate * gelu_slope
    d_up_b = (hidden_grad[:rows] * gelu_value[:rows]).astype(jnp.bfloat16)
    d_up_a = sum(
        (taps_own[i][None, :] * d_conv[span - i : span - i + rows] for i in range(TAPS))
    ).astype(jnp.bfloat16)
    own = d_conv[:rows]
    sums = [jnp.sum(own * extended[i : i + rows], axis=0) for i in range(TAPS)]
    sums.append(jnp.sum(own, axis=0))

    both = jnp.concatenate([d_up_a, d_up_b], 1)
    partial = lax.dot_general(
        weights[:, : 2 * fpad], both, (((1,), (1,)), ((), ())), preferred_element_type=f32
    ).astype(jnp.bfloat16)
    part = jnp.dot(by_y, d_up_a, preferred_element_type=f32).astype(jnp.bfloat16)
    sums = jnp.stack(sums, 0)
    partial, part, sums = lax.optimization_barrier((partial, part, sums))
    part = part.reshape(ny, nz * wrows, fpad)
    part = exchange(part, "y")
    partial, part, sums = lax.optimization_barrier((partial, part, sums))
    grad_in = lax.psum_scatter(partial, TP, scatter_dimension=0, tiled=True)
    part = total(part, jnp.bfloat16).reshape(nz, wrows, fpad)
    part = exchange(part, "z")
    grad_up = total(part, f32)

    small = jnp.concatenate([jnp.sum(grad_up * grad_up, axis=0)[None], sums], 0)
    small = total(broadcast(small.reshape(1, -1), "z"), f32)
    small = total(broadcast(small, "y"), f32).reshape(TAPS + 2, fpad)
    unit_norms = small[0, :width]
    small, unit_norms, grad_in, grad_up = lax.optimization_barrier(
        (small, unit_norms, grad_in, grad_up)
    )
    columns = broadcast(small[1:].reshape(1, -1), TP).reshape(ntp, TAPS + 1, fpad)
    columns = jnp.moveaxis(columns[:, :, :width], 0, 1).reshape(TAPS + 1, ntp * width)
    return (grad_in.T, grad_up[:, :width], unit_norms, columns[:TAPS], columns[TAPS])


def solution(mesh):
    finer = Mesh(mesh.devices.reshape(12, 8, 4, 2), ("z", "y", "x", "c"))
    placed = (P(FS, TP), P(FS, TP), P(FS, TP), P(TP, FS), P(), P(), P(FS, TP))
    return jax.shard_map(
        per_device,
        mesh=finer,
        in_specs=placed,
        out_specs=(P(FS, TP), P(FS, TP), P(TP), P(), P()),
        check_vma=False,
    )
```

```python
import math

import jax
import jax.numpy as jnp
from jax import lax
from jax.sharding import Mesh
from jax.sharding import PartitionSpec as P


TAPS = 3
Y = ("y4", "y2")
FS = ("z", *Y)
TP = ("x", "c")
LANES = 128


def up_to(n, m):
    return -(-n // m) * m


def pad_to(value, dim, length):
    widths = [(0, 0)] * value.ndim
    widths[dim] = (0, length - value.shape[dim])
    return jnp.pad(value, widths)


def broadcast(value, axes):
    copies = jnp.broadcast_to(value, (lax.axis_size(axes), *value.shape))
    return lax.all_to_all(copies, axes, split_axis=0, concat_axis=0, tiled=True)


def exchange(value, axis):
    return lax.all_to_all(value, axis, split_axis=0, concat_axis=0, tiled=True)


def total(parts, kind):
    return sum(parts[i].astype(jnp.float32) for i in range(parts.shape[0])).astype(kind)


def neighbour(block, distance):
    devices = range(lax.axis_size(FS))
    route = [(i - distance, i) for i in devices if i - distance in devices]
    return lax.ppermute(block, FS, route)


def gelu_parts(value):
    normal_cdf = 0.5 * (1.0 + jax.scipy.special.erf(value / math.sqrt(2.0)))
    density = jnp.exp(-0.5 * value * value) / math.sqrt(2.0 * math.pi)
    return (value * normal_cdf, normal_cdf + value * density)


def per_device(inputs, w_conv_up, w_gate_up, w_down, taps, conv_bias, cotangent):
    span = TAPS - 1
    nz, ny = lax.axis_size("z"), lax.axis_size(Y)
    ntp = lax.axis_size(TP)
    rows, feats = inputs.shape
    wrows, width = w_conv_up.shape
    fpad = up_to(width, LANES)
    f32 = jnp.float32

    packed = jnp.concatenate(
        [pad_to(w, 1, fpad) for w in (w_conv_up, w_gate_up, w_down.T)], axis=1
    )
    over_y = broadcast(packed, Y).reshape(ny * wrows, 3 * fpad)
    weights = lax.all_gather(over_y, "z", axis=0, tiled=True)

    before = neighbour(inputs[rows - span :], 1)
    after = neighbour(jnp.concatenate([inputs[:span], cotangent[:span]], 0), -1)

    halo = pad_to(jnp.concatenate([before, after], 0), 0, LANES)
    acts = jnp.concatenate([inputs, halo, cotangent], 0).T
    acts, over_y = lax.optimization_barrier((acts, over_y))
    tokens = acts.shape[-1]
    over_tp = broadcast(broadcast(acts, "x"), "c")
    whole = jnp.moveaxis(over_tp, 0, 1).reshape(ntp * feats, tokens)
    by_y = whole[:, :rows].reshape(nz, ny, wrows, rows)
    by_y = jnp.moveaxis(by_y, 0, 1).reshape(ny * nz * wrows, rows)

    start = lax.axis_index(TP) * width
    taps_own = pad_to(lax.dynamic_slice_in_dim(taps, start, width, 1), 1, fpad)
    bias_own = pad_to(lax.dynamic_slice_in_dim(conv_bias, start, width, 0), 0, fpad)

    def over_rows(a, b):
        return lax.dot_general(a, b, (((0,), (0,)), ((), ())), preferred_element_type=f32)

    whole, by_y, taps_own, bias_own, weights = lax.optimization_barrier(
        (whole, by_y, taps_own, bias_own, weights)
    )
    ups = over_rows(whole[:, : rows + LANES], weights[:, : 2 * fpad]).astype(jnp.bfloat16)
    d_hid = over_rows(whole[:, rows:], weights[:, 2 * fpad :]).astype(jnp.bfloat16)
    up_a, up_b = ups[:, :fpad].astype(f32), ups[:, fpad:].astype(f32)
    first = rows + span
    extended = jnp.concatenate([up_a[rows:first], up_a[:rows], up_a[first : first + span]], 0)
    gate = jnp.concatenate([up_b[:rows], up_b[first : first + span]], 0)
    hidden_grad = jnp.concatenate(
        [d_hid[LANES:], d_hid[2 * span : 3 * span]], 0
    ).astype(f32)
    reach = rows + span
    conv_out = bias_own[None, :] + sum(
        (taps_own[i][None, :] * extended[i : i + reach] for i in range(TAPS))
    )
    gelu_value, gelu_slope = gelu_parts(conv_out)
    d_conv = hidden_grad * gate * gelu_slope
    d_up_b = (hidden_grad[:rows] * gelu_value[:rows]).astype(jnp.bfloat16)
    d_up_a = sum(
        (taps_own[i][None, :] * d_conv[span - i : span - i + rows] for i in range(TAPS))
    ).astype(jnp.bfloat16)
    own = d_conv[:rows]
    sums = [jnp.sum(own * extended[i : i + rows], axis=0) for i in range(TAPS)]
    sums.append(jnp.sum(own, axis=0))

    both = jnp.concatenate([d_up_a, d_up_b], 1)
    partial = lax.dot_general(
        weights[:, : 2 * fpad], both, (((1,), (1,)), ((), ())), preferred_element_type=f32
    ).astype(jnp.bfloat16)
    cut = fpad - LANES
    part = jnp.dot(by_y, d_up_a[:, :cut], preferred_element_type=f32).astype(jnp.bfloat16)
    rest = jnp.dot(whole[:, :rows], d_up_a[:, cut:], preferred_element_type=f32)
    rest = rest.astype(jnp.bfloat16)
    sums = jnp.stack(sums, 0)
    partial, part, sums = lax.optimization_barrier((partial, part, sums))
    rest = lax.psum_scatter(rest, "z", scatter_dimension=0, tiled=True)
    grad_in = lax.psum_scatter(partial, TP, scatter_dimension=0, tiled=True)
    part = part.reshape(ny, nz * wrows, cut)
    part = exchange(part, Y)
    part = total(part, jnp.bfloat16).reshape(nz, wrows, cut)
    part = exchange(part, "z")
    part = total(part, f32)
    part, rest = lax.optimization_barrier((part, rest))
    rest = exchange(rest.reshape(ny, wrows, LANES), Y)
    grad_up = jnp.concatenate([part, total(rest, f32)], 1)

    small = jnp.concatenate([jnp.sum(grad_up * grad_up, axis=0)[None], sums], 0)
    small = total(broadcast(small.reshape(1, -1), "z"), f32)
    small = total(broadcast(small, Y), f32).reshape(TAPS + 2, fpad)
    unit_norms = small[0, :width]
    small, unit_norms, grad_in, grad_up = lax.optimization_barrier(
        (small, unit_norms, grad_in, grad_up)
    )
    columns = broadcast(small[1:].reshape(1, -1), TP).reshape(ntp, TAPS + 1, fpad)
    columns = jnp.moveaxis(columns[:, :, :width], 0, 1).reshape(TAPS + 1, ntp * width)
    return (grad_in.T, grad_up[:, :width], unit_norms, columns[:TAPS], columns[TAPS])


def solution(mesh):
    finer = Mesh(mesh.devices.reshape(12, 4, 2, 4, 2), ("z", *Y, *TP))
    placed = (P(FS, TP), P(FS, TP), P(FS, TP), P(TP, FS), P(), P(), P(FS, TP))
    return jax.shard_map(
        per_device,
        mesh=finer,
        in_specs=placed,
        out_specs=(P(FS, TP), P(FS, TP), P(TP), P(), P()),
        check_vma=False,
    )
```

```python
import math

import jax
import jax.numpy as jnp
from jax import lax
from jax.sharding import Mesh
from jax.sharding import PartitionSpec as P

TAPS = 3
FS = ("z", "y")
TP = ("x", "c")
LANES = 128


def up_to(n, m):
    return -(-n // m) * m


def pad_to(value, dim, length):
    widths = [(0, 0)] * value.ndim
    widths[dim] = (0, length - value.shape[dim])
    return jnp.pad(value, widths)


def broadcast(value, axes):
    copies = jnp.broadcast_to(value, (lax.axis_size(axes), *value.shape))
    return lax.all_to_all(copies, axes, split_axis=0, concat_axis=0, tiled=True)


def exchange(value, axis):
    return lax.all_to_all(value, axis, split_axis=0, concat_axis=0, tiled=True)


def total(parts, kind):
    return sum(parts[i].astype(jnp.float32) for i in range(parts.shape[0])).astype(kind)


def neighbour(block, distance):
    devices = range(lax.axis_size(FS))
    route = [(i - distance, i) for i in devices if i - distance in devices]
    return lax.ppermute(block, FS, route)


def gelu_parts(value):
    normal_cdf = 0.5 * (1.0 + jax.scipy.special.erf(value / math.sqrt(2.0)))
    density = jnp.exp(-0.5 * value * value) / math.sqrt(2.0 * math.pi)
    return (value * normal_cdf, normal_cdf + value * density)


def per_device(inputs, w_conv_up, w_gate_up, w_down, taps, conv_bias, cotangent):
    span = TAPS - 1
    nz, ny = lax.axis_size("z"), lax.axis_size("y")
    ntp = lax.axis_size(TP)
    rows, feats = inputs.shape
    wrows, width = w_conv_up.shape
    fpad = up_to(width, LANES)
    f32 = jnp.float32

    packed = jnp.concatenate(
        [pad_to(w, 1, fpad) for w in (w_conv_up, w_gate_up, w_down.T)], axis=1
    )
    over_y = broadcast(packed, "y").reshape(ny * wrows, 3 * fpad)
    weights = lax.all_gather(over_y, "z", axis=0, tiled=True)

    before = neighbour(inputs[rows - span :], 1)
    after = neighbour(jnp.concatenate([inputs[:span], cotangent[:span]], 0), -1)

    halo = pad_to(jnp.concatenate([before, after], 0), 0, LANES)
    acts = jnp.concatenate([inputs, halo, cotangent], 0).T
    acts, over_y = lax.optimization_barrier((acts, over_y))
    tokens = acts.shape[-1]
    over_tp = broadcast(broadcast(acts, "x"), "c")
    whole = jnp.moveaxis(over_tp, 0, 1).reshape(ntp * feats, tokens)
    by_y = whole[:, :rows].reshape(nz, ny, wrows, rows)
    by_y = jnp.moveaxis(by_y, 0, 1).reshape(ny * nz * wrows, rows)

    start = lax.axis_index(TP) * width
    taps_own = pad_to(lax.dynamic_slice_in_dim(taps, start, width, 1), 1, fpad)
    bias_own = pad_to(lax.dynamic_slice_in_dim(conv_bias, start, width, 0), 0, fpad)

    def over_rows(a, b):
        return lax.dot_general(a, b, (((0,), (0,)), ((), ())), preferred_element_type=f32)

    whole, by_y, taps_own, bias_own, weights = lax.optimization_barrier(
        (whole, by_y, taps_own, bias_own, weights)
    )
    ups = over_rows(whole[:, : rows + LANES], weights[:, : 2 * fpad]).astype(jnp.bfloat16)
    d_hid = over_rows(whole[:, rows:], weights[:, 2 * fpad :]).astype(jnp.bfloat16)
    up_a, up_b = ups[:, :fpad].astype(f32), ups[:, fpad:].astype(f32)
    first = rows + span
    extended = jnp.concatenate([up_a[rows:first], up_a[:rows], up_a[first : first + span]], 0)
    gate = jnp.concatenate([up_b[:rows], up_b[first : first + span]], 0)
    hidden_grad = jnp.concatenate(
        [d_hid[LANES:], d_hid[2 * span : 3 * span]], 0
    ).astype(f32)
    reach = rows + span
    conv_out = bias_own[None, :] + sum(
        (taps_own[i][None, :] * extended[i : i + reach] for i in range(TAPS))
    )
    gelu_value, gelu_slope = gelu_parts(conv_out)
    d_conv = hidden_grad * gate * gelu_slope
    d_up_b = (hidden_grad[:rows] * gelu_value[:rows]).astype(jnp.bfloat16)
    d_up_a = sum(
        (taps_own[i][None, :] * d_conv[span - i : span - i + rows] for i in range(TAPS))
    ).astype(jnp.bfloat16)
    own = d_conv[:rows]
    sums = [jnp.sum(own * extended[i : i + rows], axis=0) for i in range(TAPS)]
    sums.append(jnp.sum(own, axis=0))

    part = jnp.dot(by_y, d_up_a, preferred_element_type=f32).astype(jnp.bfloat16)
    part = lax.psum_scatter(part, "y", scatter_dimension=0, tiled=True)

    both = jnp.concatenate([d_up_a, d_up_b], 1)
    partial = lax.dot_general(
        weights[:, : 2 * fpad], both, (((1,), (1,)), ((), ())), preferred_element_type=f32
    ).astype(jnp.bfloat16)
    partial, sums = lax.optimization_barrier((partial, jnp.stack(sums, 0)))
    grad_in = lax.psum_scatter(partial, TP, scatter_dimension=0, tiled=True)

    sums = broadcast(sums.reshape(1, -1), "z")
    sums = broadcast(total(sums, f32), "y")
    sums = broadcast(total(sums, f32), TP).reshape(ntp, TAPS + 1, fpad)
    columns = jnp.moveaxis(sums[:, :, :width], 0, 1).reshape(TAPS + 1, ntp * width)
    grad_taps, grad_bias = columns[:TAPS], columns[TAPS]
    part, grad_taps, grad_bias = lax.optimization_barrier((part, grad_taps, grad_bias))

    part = exchange(part.reshape(nz, wrows, fpad), "z")
    grad_up = total(part, f32)
    squares = jnp.sum(grad_up * grad_up, axis=0)[None]
    grad_up, squares = lax.optimization_barrier((grad_up, squares))
    unit_norms = jnp.sum(broadcast(squares, FS), axis=(0, 1))[:width]
    unit_norms, grad_in = lax.optimization_barrier((unit_norms, grad_in))
    return (grad_in.T, grad_up[:, :width], unit_norms, grad_taps, grad_bias)


def solution(mesh):
    finer = Mesh(mesh.devices.reshape(12, 8, 4, 2), ("z", "y", "x", "c"))
    placed = (P(FS, TP), P(FS, TP), P(FS, TP), P(TP, FS), P(), P(), P(FS, TP))
    return jax.shard_map(
        per_device,
        mesh=finer,
        in_specs=placed,
        out_specs=(P(FS, TP), P(FS, TP), P(TP), P(), P()),
        check_vma=False,
    )
```

```python
import math

import jax
import jax.numpy as jnp
from jax import lax
from jax.sharding import Mesh
from jax.sharding import PartitionSpec as P

TAPS = 3
FS = ("z", "y")
TP = ("x", "c")
LANES = 128


def up_to(n, m):
    return -(-n // m) * m


def pad_to(value, dim, length):
    widths = [(0, 0)] * value.ndim
    widths[dim] = (0, length - value.shape[dim])
    return jnp.pad(value, widths)


def broadcast(value, axes):
    copies = jnp.broadcast_to(value, (lax.axis_size(axes), *value.shape))
    return lax.all_to_all(copies, axes, split_axis=0, concat_axis=0, tiled=True)


def exchange(value, axis):
    return lax.all_to_all(value, axis, split_axis=0, concat_axis=0, tiled=True)


def total(parts, kind):
    return sum(parts[i].astype(jnp.float32) for i in range(parts.shape[0])).astype(kind)


def neighbour(block, distance):
    devices = range(lax.axis_size(FS))
    route = [(i - distance, i) for i in devices if i - distance in devices]
    return lax.ppermute(block, FS, route)


def gelu_parts(value):
    normal_cdf = 0.5 * (1.0 + jax.scipy.special.erf(value / math.sqrt(2.0)))
    density = jnp.exp(-0.5 * value * value) / math.sqrt(2.0 * math.pi)
    return (value * normal_cdf, normal_cdf + value * density)


def per_device(inputs, w_conv_up, w_gate_up, w_down, taps, conv_bias, cotangent):
    span = TAPS - 1
    nz, ny = lax.axis_size("z"), lax.axis_size("y")
    ntp = lax.axis_size(TP)
    rows, feats = inputs.shape
    wrows, width = w_conv_up.shape
    fpad = up_to(width, LANES)
    f32 = jnp.float32

    packed = jnp.concatenate(
        [pad_to(w, 1, fpad) for w in (w_conv_up, w_gate_up, w_down.T)], axis=1
    )
    over_y = broadcast(packed, "y").reshape(ny * wrows, 3 * fpad)
    weights = lax.all_gather(over_y, "z", axis=0, tiled=True)

    before = neighbour(inputs[rows - span :], 1)
    after = neighbour(jnp.concatenate([inputs[:span], cotangent[:span]], 0), -1)

    halo = pad_to(jnp.concatenate([before, after], 0), 0, LANES)
    acts = jnp.concatenate([inputs, halo, cotangent], 0).T
    acts, over_y = lax.optimization_barrier((acts, over_y))
    tokens = acts.shape[-1]
    over_tp = broadcast(broadcast(acts, "x"), "c")
    whole = jnp.moveaxis(over_tp, 0, 1).reshape(ntp * feats, tokens)
    by_y = whole[:, :rows].reshape(nz, ny, wrows, rows)
    by_y = jnp.moveaxis(by_y, 0, 1).reshape(ny * nz * wrows, rows)

    start = lax.axis_index(TP) * width
    taps_own = pad_to(lax.dynamic_slice_in_dim(taps, start, width, 1), 1, fpad)
    bias_own = pad_to(lax.dynamic_slice_in_dim(conv_bias, start, width, 0), 0, fpad)

    def over_rows(a, b):
        return lax.dot_general(a, b, (((0,), (0,)), ((), ())), preferred_element_type=f32)

    ahead, behind = whole[:, : rows + 8], whole[:, rows:]
    ahead, behind, by_y, taps_own, bias_own, weights = lax.optimization_barrier(
        (ahead, behind, by_y, taps_own, bias_own, weights)
    )
    ups = over_rows(ahead, weights[:, : 2 * fpad]).astype(jnp.bfloat16)
    d_hid = over_rows(behind, weights[:, 2 * fpad :]).astype(jnp.bfloat16)
    up_a, up_b = ups[:, :fpad].astype(f32), ups[:, fpad:].astype(f32)
    first = rows + span
    extended = jnp.concatenate([up_a[rows:first], up_a[:rows], up_a[first : first + span]], 0)
    gate = jnp.concatenate([up_b[:rows], up_b[first : first + span]], 0)
    hidden_grad = jnp.concatenate(
        [d_hid[LANES:], d_hid[2 * span : 3 * span]], 0
    ).astype(f32)
    reach = rows + span
    conv_out = bias_own[None, :] + sum(
        (taps_own[i][None, :] * extended[i : i + reach] for i in range(TAPS))
    )
    gelu_value, gelu_slope = gelu_parts(conv_out)
    d_conv = hidden_grad * gate * gelu_slope
    d_up_b = (hidden_grad[:rows] * gelu_value[:rows]).astype(jnp.bfloat16)
    d_up_a = sum(
        (taps_own[i][None, :] * d_conv[span - i : span - i + rows] for i in range(TAPS))
    ).astype(jnp.bfloat16)
    own = d_conv[:rows]
    sums = [jnp.sum(own * extended[i : i + rows], axis=0) for i in range(TAPS)]
    sums.append(jnp.sum(own, axis=0))

    part = jnp.dot(by_y, d_up_a, preferred_element_type=f32).astype(jnp.bfloat16)
    part = lax.psum_scatter(part, "y", scatter_dimension=0, tiled=True)

    both = jnp.concatenate([d_up_a, d_up_b], 1)
    partial = lax.dot_general(
        weights[:, : 2 * fpad], both, (((1,), (1,)), ((), ())), preferred_element_type=f32
    ).astype(jnp.bfloat16)
    partial, sums = lax.optimization_barrier((partial, jnp.stack(sums, 0)))
    grad_in = lax.psum_scatter(partial, TP, scatter_dimension=0, tiled=True)

    sums = broadcast(sums.reshape(1, -1), "z")
    sums = broadcast(total(sums, f32), "y")
    sums = broadcast(total(sums, f32), TP).reshape(ntp, TAPS + 1, fpad)
    columns = jnp.moveaxis(sums[:, :, :width], 0, 1).reshape(TAPS + 1, ntp * width)
    grad_taps, grad_bias = columns[:TAPS], columns[TAPS]
    part, grad_taps, grad_bias = lax.optimization_barrier((part, grad_taps, grad_bias))

    part = exchange(part.reshape(nz, wrows, fpad), "z")
    grad_up = total(part, f32)
    squares = jnp.sum(grad_up * grad_up, axis=0)[None]
    grad_up, squares = lax.optimization_barrier((grad_up, squares))
    unit_norms = jnp.sum(broadcast(squares, FS), axis=(0, 1))[:width]
    unit_norms, grad_in = lax.optimization_barrier((unit_norms, grad_in))
    return (grad_in.T, grad_up[:, :width], unit_norms, grad_taps, grad_bias)


def solution(mesh):
    finer = Mesh(mesh.devices.reshape(12, 8, 4, 2), ("z", "y", "x", "c"))
    placed = (P(FS, TP), P(FS, TP), P(FS, TP), P(TP, FS), P(), P(), P(FS, TP))
    return jax.shard_map(
        per_device,
        mesh=finer,
        in_specs=placed,
        out_specs=(P(FS, TP), P(FS, TP), P(TP), P(), P()),
        check_vma=False,
    )
```

```python
import math

import jax
import jax.numpy as jnp
from jax import lax
from jax.experimental import pallas as pl
from jax.sharding import Mesh
from jax.sharding import PartitionSpec as P

TAPS = 3
FS = ("z", "y")
TP = ("x", "c")
LANES = 128


def up_to(n, m):
    return -(-n // m) * m


def pad_to(value, dim, length):
    widths = [(0, 0)] * value.ndim
    widths[dim] = (0, length - value.shape[dim])
    return jnp.pad(value, widths)


def broadcast(value, axes):
    copies = jnp.broadcast_to(value, (lax.axis_size(axes), *value.shape))
    return lax.all_to_all(copies, axes, split_axis=0, concat_axis=0, tiled=True)


def exchange(value, axis):
    return lax.all_to_all(value, axis, split_axis=0, concat_axis=0, tiled=True)


def total(parts, kind):
    return sum(parts[i].astype(jnp.float32) for i in range(parts.shape[0])).astype(kind)


def neighbour(block, distance):
    devices = range(lax.axis_size(FS))
    route = [(i - distance, i) for i in devices if i - distance in devices]
    return lax.ppermute(block, FS, route)


def input_part(weights, both):
    rows, depth = both.shape
    features = weights.shape[0]
    block = next(n for n in range(352, 0, -16) if features % n == 0)

    def kernel(weights_ref, both_ref, out_ref):
        out_ref[...] = lax.dot_general(
            weights_ref[...],
            both_ref[...],
            (((1,), (1,)), ((), ())),
            preferred_element_type=jnp.float32,
        ).astype(out_ref.dtype)

    return pl.pallas_call(
        kernel,
        grid=(features // block,),
        in_specs=[
            pl.BlockSpec((block, depth), lambda i: (i, 0)),
            pl.BlockSpec((rows, depth), lambda i: (0, 0)),
        ],
        out_specs=pl.BlockSpec((block, rows), lambda i: (i, 0)),
        out_shape=jax.ShapeDtypeStruct((features, rows), weights.dtype),
        cost_estimate=pl.CostEstimate(
            flops=2 * features * depth * rows,
            bytes_accessed=2 * (features * depth + rows * depth + features * rows),
            transcendentals=0,
        ),
    )(weights, both)


def gelu_parts(value):
    normal_cdf = 0.5 * (1.0 + jax.scipy.special.erf(value / math.sqrt(2.0)))
    density = jnp.exp(-0.5 * value * value) / math.sqrt(2.0 * math.pi)
    return (value * normal_cdf, normal_cdf + value * density)


def per_device(inputs, w_conv_up, w_gate_up, w_down, taps, conv_bias, cotangent):
    span = TAPS - 1
    nz, ny = lax.axis_size("z"), lax.axis_size("y")
    ntp = lax.axis_size(TP)
    rows, feats = inputs.shape
    wrows, width = w_conv_up.shape
    fpad = up_to(width, LANES)
    f32 = jnp.float32

    packed = jnp.concatenate(
        [pad_to(w, 1, fpad) for w in (w_conv_up, w_gate_up, w_down.T)], axis=1
    )
    over_y = broadcast(packed, "y").reshape(ny * wrows, 3 * fpad)
    weights = lax.all_gather(over_y, "z", axis=0, tiled=True)

    before = neighbour(inputs[rows - span :], 1)
    after = neighbour(jnp.concatenate([inputs[:span], cotangent[:span]], 0), -1)

    halo = pad_to(jnp.concatenate([before, after], 0), 0, LANES)
    acts = jnp.concatenate([inputs, halo, cotangent], 0).T
    acts, over_y = lax.optimization_barrier((acts, over_y))
    tokens = acts.shape[-1]
    over_tp = broadcast(broadcast(acts, "x"), "c")
    whole = jnp.moveaxis(over_tp, 0, 1).reshape(ntp * feats, tokens)
    by_y = whole[:, :rows].reshape(nz, ny, wrows, rows)
    by_y = jnp.moveaxis(by_y, 0, 1).reshape(ny * nz * wrows, rows)

    start = lax.axis_index(TP) * width
    taps_own = pad_to(lax.dynamic_slice_in_dim(taps, start, width, 1), 1, fpad)
    bias_own = pad_to(lax.dynamic_slice_in_dim(conv_bias, start, width, 0), 0, fpad)

    def over_rows(a, b):
        return lax.dot_general(a, b, (((0,), (0,)), ((), ())), preferred_element_type=f32)

    ahead, behind = whole[:, : rows + 8], whole[:, rows:]
    ahead, behind, by_y, taps_own, bias_own, weights = lax.optimization_barrier(
        (ahead, behind, by_y, taps_own, bias_own, weights)
    )
    ups = over_rows(ahead, weights[:, : 2 * fpad]).astype(jnp.bfloat16)
    d_hid = over_rows(behind, weights[:, 2 * fpad :]).astype(jnp.bfloat16)
    up_a, up_b = ups[:, :fpad].astype(f32), ups[:, fpad:].astype(f32)
    first = rows + span
    extended = jnp.concatenate([up_a[rows:first], up_a[:rows], up_a[first : first + span]], 0)
    gate = jnp.concatenate([up_b[:rows], up_b[first : first + span]], 0)
    hidden_grad = jnp.concatenate(
        [d_hid[LANES:], d_hid[2 * span : 3 * span]], 0
    ).astype(f32)
    reach = rows + span
    conv_out = bias_own[None, :] + sum(
        (taps_own[i][None, :] * extended[i : i + reach] for i in range(TAPS))
    )
    gelu_value, gelu_slope = gelu_parts(conv_out)
    d_conv = hidden_grad * gate * gelu_slope
    d_up_b = (hidden_grad[:rows] * gelu_value[:rows]).astype(jnp.bfloat16)
    d_up_a = sum(
        (taps_own[i][None, :] * d_conv[span - i : span - i + rows] for i in range(TAPS))
    ).astype(jnp.bfloat16)
    own = d_conv[:rows]
    sums = [jnp.sum(own * extended[i : i + rows], axis=0) for i in range(TAPS)]
    sums.append(jnp.sum(own, axis=0))

    part = jnp.dot(by_y, d_up_a, preferred_element_type=f32).astype(jnp.bfloat16)
    part = lax.psum_scatter(part, "y", scatter_dimension=0, tiled=True)

    both = jnp.concatenate([d_up_a, d_up_b], 1)
    partial = input_part(weights, both)
    partial, sums = lax.optimization_barrier((partial, jnp.stack(sums, 0)))
    grad_in = lax.psum_scatter(partial, TP, scatter_dimension=0, tiled=True)

    sums = broadcast(sums.reshape(1, -1), "z")
    sums = broadcast(total(sums, f32), "y")
    sums = broadcast(total(sums, f32), TP).reshape(ntp, TAPS + 1, fpad)
    columns = jnp.moveaxis(sums[:, :, :width], 0, 1).reshape(TAPS + 1, ntp * width)
    grad_taps, grad_bias = columns[:TAPS], columns[TAPS]
    part, grad_taps, grad_bias = lax.optimization_barrier((part, grad_taps, grad_bias))

    part = exchange(part.reshape(nz, wrows, fpad), "z")
    grad_up = total(part, f32)
    squares = jnp.sum(grad_up * grad_up, axis=0)[None]
    grad_up, squares = lax.optimization_barrier((grad_up, squares))
    unit_norms = jnp.sum(broadcast(squares, FS), axis=(0, 1))[:width]
    unit_norms, grad_in = lax.optimization_barrier((unit_norms, grad_in))
    return (grad_in.T, grad_up[:, :width], unit_norms, grad_taps, grad_bias)


def solution(mesh):
    finer = Mesh(mesh.devices.reshape(12, 8, 4, 2), ("z", "y", "x", "c"))
    placed = (P(FS, TP), P(FS, TP), P(FS, TP), P(TP, FS), P(), P(), P(FS, TP))
    return jax.shard_map(
        per_device,
        mesh=finer,
        in_specs=placed,
        out_specs=(P(FS, TP), P(FS, TP), P(TP), P(), P()),
        check_vma=False,
    )
```
